32 devices in a mesh: rep: 2 (over x), fs: 8 (over z, y), tp: 2 (over core).
Axes of the slice: x: 2, y: 2, z: 4, core: 2. Of those that a mesh axis runs over, the one named last changes fastest.
Arguments:
- tokens: bfloat16 [2048, 2048], P(('rep', 'fs')), may hold values from -6 to 6
- attention_norm_gain: float32 [2048], replicated, may hold values from 0.1 to 1.9
- query_weight: bfloat16 [2048, 1024], P('fs', 'tp'), may hold values from -0.125 to 0.125
- key_weight: bfloat16 [2048, 1024], P('fs', 'tp'), may hold values from -0.125 to 0.125
- value_weight: bfloat16 [2048, 2048], P('fs', 'tp'), may hold values from -0.125 to 0.125
- decay_weight: bfloat16 [2048, 1024], P('fs', 'tp'), may hold values from -0.125 to 0.125
- decay_gate_bias: float32 [1024], P('tp'), may hold values from -1.5 to 5.5
- decay_spike_extra: float32 [2048, 32], P(('rep', 'fs'), 'tp'), may hold values from -0.7 to 0
- head_output_gain: float32 [64], replicated, may hold values from 0.1 to 1.9
- output_weight: bfloat16 [2048, 2048], P('fs', 'tp'), may hold values from -0.125 to 0.125
- channel_norm_gain: float32 [2048], replicated, may hold values from 0.1 to 1.9
- gate_weight: bfloat16 [2048, 3072], P('fs', 'tp'), may hold values from -0.125 to 0.125
- up_weight: bfloat16 [2048, 3072], P('fs', 'tp'), may hold values from -0.125 to 0.125
- down_weight: bfloat16 [2048, 3072], P('fs', 'tp'), may hold values from -0.109375 to 0.109375
Outputs:
- layer_out: bfloat16 [2048, 2048], P(('rep', 'fs'))
The draws below stay inside these ranges and needn't reach their ends.
All inputs are finite; a program needn't handle non-finite values.
Results may differ from the reference program's by a relative error of at most 0.018.
Values may be sent and summed in bfloat16 or wider, within the bound.
No kernel may reach another device: no remote copies, remote signals or barrier semaphores. Data moves between devices by JAX's collectives and lax.ppermute only.
A program may use at most 128 MiB of HBM per device.

```python
import jax
import jax.numpy as jnp
from jax import lax

D = 2048
HEAD_K = 32
HEAD_V = 64
HEADS = 32
FF = 3072
BLOCK = 64
TOK_GROUP = 128
TOKENS = 2048
N_TP = 2


def draw_decay_gate_bias(key, part):
    keys_all = jax.random.split(key, 4)
    fast_share = 0.5
    is_fast = jax.random.uniform(keys_all[0], (HEADS,), jnp.float32) < fast_share
    fast_value = jax.random.uniform(keys_all[1], (HEADS,), jnp.float32, -1.0, 0.0)
    slow_value = jax.random.uniform(keys_all[2], (HEADS,), jnp.float32, 3.0, 5.0)
    base_value = jnp.where(is_fast, fast_value, slow_value)
    jitter = jax.random.uniform(keys_all[3], (HEADS, HEAD_K), jnp.float32, -0.5, 0.5)
    return (base_value[:, None] + jitter).reshape(HEADS * HEAD_K).astype(jnp.float32)


def draw_decay_spike_extra(key, part):
    keys_all = jax.random.split(key, 2)
    chosen = jax.random.uniform(keys_all[0], (TOKENS, HEADS), jnp.float32) < 3.0 / TOK_GROUP
    depth = jax.random.uniform(keys_all[1], (TOKENS, HEADS), jnp.float32, -0.7, -0.22)
    return jnp.where(chosen, depth, 0.0).astype(jnp.float32)


def levels(own_key, extent, cuts, smallest, high):
    loudness, own = 1.0, jax.random.fold_in(own_key, 6)
    for position, blocks in cuts:
        draws = jnp.exp(jax.random.uniform(jax.random.fold_in(own, position), (blocks,), jnp.float32, smallest / len(cuts), high / len(cuts)))
        loudness = loudness * jnp.repeat(draws, extent[position] // blocks).reshape([-1 if axis == position else 1 for axis in range(len(extent))])
    return loudness


def bell_draw(own_key, extent, deviation, bound, shards=(), kind=jnp.bfloat16):
    values = deviation * jax.random.normal(own_key, extent, jnp.float32)
    if shards:
        values = values * levels(own_key, extent, shards, -0.22, 0.18)
    return jnp.clip(values, -bound, bound).astype(kind)


def setup_inputs(seed: int = 0) -> dict:
    seeds = jax.random.split(jax.random.key(seed), 15)
    return {
        "tokens": bell_draw(seeds[0], (TOKENS, D), 1.0, 6.0, ((0, 16),)),
        "attention_norm_gain": jnp.clip(1.0 + 0.18 * jax.random.normal(seeds[1], (D,), jnp.float32), 0.1, 1.9),
        "query_weight": bell_draw(seeds[2], (D, HEADS * HEAD_K), D ** -0.5, 0.125, ((0, 8), (1, 2))),
        "key_weight": bell_draw(seeds[3], (D, HEADS * HEAD_K), D ** -0.5, 0.125, ((0, 8), (1, 2))),
        "value_weight": bell_draw(seeds[4], (D, HEADS * HEAD_V), D ** -0.5, 0.125, ((0, 8), (1, 2))),
        "decay_weight": bell_draw(seeds[5], (D, HEADS * HEAD_K), D ** -0.5, 0.125, ((0, 8), (1, 2))),
        "decay_gate_bias": draw_decay_gate_bias(jax.random.fold_in(seeds[14], 71), 0),
        "decay_spike_extra": draw_decay_spike_extra(jax.random.fold_in(seeds[14], 71), 0),
        "head_output_gain": jnp.clip(1.0 + 0.18 * jax.random.normal(seeds[8], (HEAD_V,), jnp.float32), 0.1, 1.9),
        "output_weight": bell_draw(seeds[9], (D, HEADS * HEAD_V), (HEADS * HEAD_V) ** -0.5, 0.125, ((0, 8), (1, 2))),
        "channel_norm_gain": jnp.clip(1.0 + 0.18 * jax.random.normal(seeds[10], (D,), jnp.float32), 0.1, 1.9),
        "gate_weight": bell_draw(seeds[11], (D, FF), D ** -0.5, 0.125, ((0, 8), (1, 2))),
        "up_weight": bell_draw(seeds[12], (D, FF), D ** -0.5, 0.125, ((0, 8), (1, 2))),
        "down_weight": bell_draw(seeds[13], (D, FF), FF ** -0.5, 0.109375, ((0, 8), (1, 2))),
    }


GATE_NORM = 16.0
NORM_EPS = 1e-06
HIGHEST = lax.Precision.HIGHEST

def rms_scale(values, scales):
    floats = values.astype(jnp.float32)
    return floats * lax.rsqrt(lax.optimization_barrier(jnp.mean(floats * floats, axis=-1, keepdims=True)) + NORM_EPS) * scales

def one_way(queries, key_rows, value_rows, decay_logarithm):
    length, number_of_heads, key_width = queries.shape
    value_width = value_rows.shape[2]
    block_count = length // BLOCK

    def blocks(tensor):
        return tensor.reshape(block_count, BLOCK, number_of_heads, tensor.shape[2]).transpose(0, 2, 1, 3)
    lower_mask = jnp.tril(jnp.ones((BLOCK, BLOCK), bool))

    def advance(carried, pieces):
        query_part, key_part, value_part, decay_part = pieces
        running = jnp.cumsum(decay_part, axis=1)
        spread = jnp.where(lower_mask[None, :, :, None], running[:, :, None, :] - running[:, None, :, :], -jnp.inf)
        scores = jnp.einsum('hid,hjd,hijd->hij', query_part, key_part, jnp.exp(spread), precision=HIGHEST)
        block_end = running[:, -1:, :]
        result = jnp.einsum('hij,hje->hie', scores, value_part, precision=HIGHEST)
        result = result + jnp.einsum('hid,hde->hie', query_part * jnp.exp(running), carried, precision=HIGHEST)
        carried = jnp.exp(block_end)[:, 0, :, None] * carried + jnp.einsum('hjd,hje->hde', key_part * jnp.exp(block_end - running), value_part, precision=HIGHEST)
        return (carried, result)
    zero_state = jnp.zeros((number_of_heads, key_width, value_width), jnp.float32)
    _, outputs = lax.scan(advance, zero_state, (blocks(queries), blocks(key_rows), blocks(value_rows), blocks(decay_logarithm)))
    return outputs.transpose(0, 2, 1, 3).reshape(length, number_of_heads, value_width)

def both_ways(queries, key_rows, value_rows, decay_logarithm):
    forward = one_way(queries, key_rows, value_rows, decay_logarithm)
    backward = one_way(jnp.flip(queries, 0), jnp.flip(key_rows, 0), jnp.flip(value_rows, 0), jnp.flip(decay_logarithm, 0))
    return forward + jnp.flip(backward, 0)

def rounded(floats):
    return lax.optimization_barrier(floats.astype(jnp.bfloat16)).astype(jnp.float32)

def grouped_sum(left, right):
    width = left.shape[1] // N_TP
    total = jnp.zeros((left.shape[0], right.shape[0]), jnp.float32)
    for shard_id in range(N_TP):
        part_left = left[:, shard_id * width:(shard_id + 1) * width]
        part_right = right[:, shard_id * width:(shard_id + 1) * width]
        partial_sum = lax.dot_general(part_left, part_right, (((1,), (1,)), ((), ())), preferred_element_type=jnp.float32)
        total = total + rounded(partial_sum)
    return total

def reference(tokens, attention_norm_gain, query_weight, key_weight, value_weight, decay_weight, decay_gate_bias, decay_spike_extra, head_output_gain, output_weight, channel_norm_gain, gate_weight, up_weight, down_weight):
    normed = rms_scale(tokens, attention_norm_gain).astype(jnp.bfloat16)
    queries = jnp.dot(normed, query_weight, preferred_element_type=jnp.float32).astype(jnp.bfloat16)
    key_rows = jnp.dot(normed, key_weight, preferred_element_type=jnp.float32).astype(jnp.bfloat16)
    value_rows = jnp.dot(normed, value_weight, preferred_element_type=jnp.float32).astype(jnp.bfloat16)
    gate_pre = jnp.dot(normed, decay_weight, preferred_element_type=jnp.float32)
    decay_logarithm = jax.nn.log_sigmoid(gate_pre + decay_gate_bias).reshape(TOKENS, HEADS, HEAD_K) / GATE_NORM
    decay_logarithm = decay_logarithm + decay_spike_extra[:, :, None]
    seq_count = TOKENS // TOK_GROUP
    query_seq = (queries.astype(jnp.float32) * HEAD_K ** (-0.5)).reshape(seq_count, TOK_GROUP, HEADS, HEAD_K)
    key_seq = key_rows.astype(jnp.float32).reshape(seq_count, TOK_GROUP, HEADS, HEAD_K)
    value_seq = value_rows.astype(jnp.float32).reshape(seq_count, TOK_GROUP, HEADS, HEAD_V)
    decay_seq = decay_logarithm.reshape(seq_count, TOK_GROUP, HEADS, HEAD_K)

    def attend(pieces):
        mixed_heads = both_ways(*pieces)
        normed_heads = rms_scale(mixed_heads, head_output_gain)
        return normed_heads.reshape(TOK_GROUP, HEADS * HEAD_V).astype(jnp.bfloat16)
    attended = lax.map(attend, (query_seq, key_seq, value_seq, decay_seq)).reshape(TOKENS, HEADS * HEAD_V)
    residual = (tokens.astype(jnp.float32) + grouped_sum(attended, output_weight)).astype(jnp.bfloat16)
    normed_two = rms_scale(residual, channel_norm_gain).astype(jnp.bfloat16)
    gate_pre_two = jnp.dot(normed_two, gate_weight, preferred_element_type=jnp.float32)
    up_proj = jnp.dot(normed_two, up_weight, preferred_element_type=jnp.float32)
    hidden = (jax.nn.silu(gate_pre_two) * up_proj).astype(jnp.bfloat16)
    return (residual.astype(jnp.float32) + grouped_sum(hidden, down_weight)).astype(jnp.bfloat16)
```

```python
import functools

import jax
import jax.numpy as jnp
from jax import lax
from jax.experimental import pallas as pl
from jax.experimental.pallas import tpu as pltpu
from jax.sharding import PartitionSpec as P

BLOCK = 64


GATE_NORM = 16.0
NORM_EPS = 1e-06
HIGHEST = lax.Precision.HIGHEST
LINE = 4
VMEM_LIMIT = 40 * 1024 * 1024


def rms_scale(values, scales):
    floats = values.astype(jnp.float32)
    return floats * lax.rsqrt(jnp.mean(floats * floats, axis=-1, keepdims=True) + NORM_EPS) * scales


def one_way(queries, key_rows, value_rows, decay_logarithm):
    length, number_of_heads, key_width = queries.shape
    value_width = value_rows.shape[2]
    block_count = length // BLOCK

    def blocks(tensor):
        return tensor.reshape(block_count, BLOCK, number_of_heads, tensor.shape[2]).transpose(
            0, 2, 1, 3
        )

    lower_mask = jnp.tril(jnp.ones((BLOCK, BLOCK), bool))

    def advance(carried, pieces):
        query_part, key_part, value_part, decay_part = pieces
        running = jnp.cumsum(decay_part, axis=1)
        spread = jnp.where(
            lower_mask[None, :, :, None], running[:, :, None, :] - running[:, None, :, :], -jnp.inf
        )
        scores = jnp.einsum(
            "hid,hjd,hijd->hij", query_part, key_part, jnp.exp(spread), precision=HIGHEST
        )
        block_end = running[:, -1:, :]
        result = jnp.einsum("hij,hje->hie", scores, value_part, precision=HIGHEST)
        result = result + jnp.einsum(
            "hid,hde->hie", query_part * jnp.exp(running), carried, precision=HIGHEST
        )
        carried = jnp.exp(block_end)[:, 0, :, None] * carried + jnp.einsum(
            "hjd,hje->hde", key_part * jnp.exp(block_end - running), value_part, precision=HIGHEST
        )
        return (carried, result)

    zero_state = jnp.zeros((number_of_heads, key_width, value_width), jnp.float32)
    _, outputs = lax.scan(
        advance,
        zero_state,
        (blocks(queries), blocks(key_rows), blocks(value_rows), blocks(decay_logarithm)),
    )
    return outputs.transpose(0, 2, 1, 3).reshape(length, number_of_heads, value_width)


def both_ways(queries, key_rows, value_rows, decay_logarithm):
    forward = one_way(queries, key_rows, value_rows, decay_logarithm)
    backward = one_way(
        jnp.flip(queries, 0),
        jnp.flip(key_rows, 0),
        jnp.flip(value_rows, 0),
        jnp.flip(decay_logarithm, 0),
    )
    return forward + jnp.flip(backward, 0)


def rounded(floats):
    return lax.optimization_barrier(floats.astype(jnp.bfloat16)).astype(jnp.float32)


def shards_general(
    tokens,
    attention_norm_gain,
    query_weight,
    key_weight,
    value_weight,
    decay_weight,
    decay_gate_bias,
    decay_spike_extra,
    head_output_gain,
    output_weight,
    channel_norm_gain,
    gate_weight,
    up_weight,
    down_weight,
):
    full_query, full_key, full_value, full_decay, full_output = (
        lax.all_gather(query_weight, "fs", axis=0, tiled=True),
        lax.all_gather(key_weight, "fs", axis=0, tiled=True),
        lax.all_gather(value_weight, "fs", axis=0, tiled=True),
        lax.all_gather(decay_weight, "fs", axis=0, tiled=True),
        lax.all_gather(output_weight, "fs", axis=0, tiled=True),
    )
    normed = rms_scale(tokens, attention_norm_gain).astype(jnp.bfloat16)
    narrow = full_query.shape[1]
    wide_cols = full_value.shape[1]
    length = normed.shape[0]
    number_of_heads = decay_spike_extra.shape[1]
    key_width = narrow // number_of_heads
    value_width = wide_cols // number_of_heads
    query_proj = jnp.dot(normed, full_query, preferred_element_type=jnp.float32)
    key_proj = jnp.dot(normed, full_key, preferred_element_type=jnp.float32)
    value_proj = jnp.dot(normed, full_value, preferred_element_type=jnp.float32)
    gate_pre = jnp.dot(normed, full_decay, preferred_element_type=jnp.float32)
    queries = (rounded(query_proj) * key_width ** (-0.5)).reshape(
        length, number_of_heads, key_width
    )
    key_rows = rounded(key_proj).reshape(length, number_of_heads, key_width)
    value_rows = rounded(value_proj).reshape(length, number_of_heads, value_width)
    decay_logarithm = (
        jax.nn.log_sigmoid(gate_pre + decay_gate_bias).reshape(length, number_of_heads, key_width)
        / GATE_NORM
    )
    decay_logarithm = decay_logarithm + decay_spike_extra[:, :, None]
    mixed_heads = both_ways(queries, key_rows, value_rows, decay_logarithm)
    attended = (
        rms_scale(mixed_heads, head_output_gain).reshape(length, wide_cols).astype(jnp.bfloat16)
    )
    full_gate, full_up, full_down = (
        lax.all_gather(gate_weight, "fs", axis=0, tiled=True),
        lax.all_gather(up_weight, "fs", axis=0, tiled=True),
        lax.all_gather(down_weight, "fs", axis=0, tiled=True),
    )
    mixer_term = lax.dot_general(
        attended, full_output, (((1,), (1,)), ((), ())), preferred_element_type=jnp.float32
    )
    mixed_sum = lax.psum(mixer_term.astype(jnp.bfloat16), "tp").astype(jnp.float32)
    residual = (tokens.astype(jnp.float32) + mixed_sum).astype(jnp.bfloat16)
    normed_two = rms_scale(residual, channel_norm_gain).astype(jnp.bfloat16)
    gate_part = jnp.dot(normed_two, full_gate, preferred_element_type=jnp.float32)
    up_part = jnp.dot(normed_two, full_up, preferred_element_type=jnp.float32)
    hidden = (jax.nn.silu(gate_part) * up_part).astype(jnp.bfloat16)
    channel_term = lax.dot_general(
        hidden, full_down, (((1,), (1,)), ((), ())), preferred_element_type=jnp.float32
    )
    channel_sum = lax.psum(channel_term.astype(jnp.bfloat16), "tp").astype(jnp.float32)
    return (residual.astype(jnp.float32) + channel_sum).astype(jnp.bfloat16)


def block_values(place_ref, blocks, line):
    first, by_mid, by_end = blocks[: line - 2], blocks[line - 2 : line], blocks[line : line + 2]
    for ref in first:
        yield ref[...]
    middle = place_ref[1] > 0
    for mid_ref, end_ref in zip(by_mid, by_end):
        yield jnp.where(middle, mid_ref[...], end_ref[...])


def project_in(place_ref, pieces, blocks, total_ref, line):
    depth = blocks[0].shape[0]
    for k, block in enumerate(block_values(place_ref, blocks, line)):
        start = pl.multiple_of((place_ref[0] ^ k) * depth, depth)
        left = jnp.concatenate([piece[:, pl.ds(start, depth)] for piece in pieces], axis=0)
        product = jnp.dot(left, block, preferred_element_type=jnp.float32)
        if k == 0:
            total_ref[...] = product
        else:
            total_ref[...] += product


def attention_kernel(line, n_seq, heads, key_width, value_width, place_ref, *refs):
    pieces, refs = refs[: 2 * n_seq], refs[2 * n_seq :]
    blocks, refs = refs[: line + 2], refs[line + 2 :]
    spikes, refs = refs[:n_seq], refs[n_seq:]
    levels_ref, bias_ref, gain_ref, out_ref, total_ref = refs
    project_in(place_ref, pieces, blocks, total_ref, line)
    half = pieces[0].shape[0]
    length = 2 * half
    wide_k, wide_v = heads * key_width, heads * value_width
    n_levels = levels_ref.shape[0]
    rows = lax.broadcasted_iota(jnp.int32, (length, length), 0)
    cols = lax.broadcasted_iota(jnp.int32, (length, length), 1)
    lane_k = lax.broadcasted_iota(jnp.int32, (length, wide_k), 1) // key_width
    lane_v = lax.broadcasted_iota(jnp.int32, (length, wide_v), 1) // value_width
    same_head = (
        lax.broadcasted_iota(jnp.int32, (wide_v, wide_v), 0) // value_width
        == lax.broadcasted_iota(jnp.int32, (wide_v, wide_v), 1) // value_width
    )
    head_ones = jnp.where(same_head, 1.0, 0.0).astype(jnp.bfloat16)
    bias = bias_ref[...]
    gain = gain_ref[...]
    for seq in range(n_seq):
        near = pl.ds(seq * half, half)
        far = pl.ds((n_seq + seq) * half, half)

        def take(low, width):
            return jnp.concatenate(
                [total_ref[near, pl.ds(low, width)], total_ref[far, pl.ds(low, width)]], axis=0
            )

        query = take(0, wide_k).astype(jnp.bfloat16).astype(jnp.float32)
        key = take(wide_k, wide_k).astype(jnp.bfloat16).astype(jnp.float32)
        value = take(2 * wide_k, wide_v).astype(jnp.bfloat16)
        gate = take(2 * wide_k + wide_v, wide_k) + bias
        decay = (
            jnp.minimum(gate, 0.0) - jnp.log(1.0 + jnp.exp(-jnp.abs(gate)))
        ) / GATE_NORM + spikes[seq][...]
        high = decay.astype(jnp.bfloat16)
        low = (decay - high.astype(jnp.float32)).astype(jnp.bfloat16)
        both = jnp.concatenate([high, low], axis=0)
        totals = [None] * heads
        for level in range(n_levels + 1):
            if level < n_levels:
                block = length >> (level + 1)
                spans = jnp.exp(
                    jnp.dot(levels_ref[level], both, preferred_element_type=jnp.float32)
                )
                left, right = query * spans[:length], key * spans[length:]
                mask = (rows // (2 * block) == cols // (2 * block)) & (
                    rows // block != cols // block
                )
                weight = 1.0
            else:
                left, right = query, key
                mask = rows == cols
                weight = 2.0
            stacked = jnp.concatenate(
                [jnp.where(lane_k == h, left, 0.0).astype(jnp.bfloat16) for h in range(heads)],
                axis=0,
            )
            scores = lax.dot_general(
                stacked,
                right.astype(jnp.bfloat16),
                (((1,), (1,)), ((), ())),
                preferred_element_type=jnp.float32,
            )
            for h in range(heads):
                term = jnp.where(mask, scores[h * length : (h + 1) * length] * weight, 0.0)
                totals[h] = term if level == 0 else totals[h] + term
        scores = jnp.concatenate(
            [(total * key_width ** (-0.5)).astype(jnp.bfloat16) for total in totals], axis=0
        )
        mixed_all = jnp.dot(scores, value, preferred_element_type=jnp.float32)
        mixed = jnp.zeros((length, wide_v), jnp.float32)
        for h in range(heads):
            mixed = jnp.where(lane_v == h, mixed_all[h * length : (h + 1) * length], mixed)
        square = mixed * mixed
        square_high = square.astype(jnp.bfloat16)
        square_low = (square - square_high.astype(jnp.float32)).astype(jnp.bfloat16)
        mean = (
            jnp.dot(square_high, head_ones, preferred_element_type=jnp.float32)
            + jnp.dot(square_low, head_ones, preferred_element_type=jnp.float32)
        ) / value_width
        attended = (mixed * lax.rsqrt(mean + NORM_EPS) * gain).astype(jnp.bfloat16)
        out_ref[near, :] = attended[:half]
        out_ref[far, :] = attended[half:]


def hidden_kernel(line, n_pieces, place_ref, *refs):
    pieces, refs = refs[:n_pieces], refs[n_pieces:]
    blocks, (out_ref, total_ref) = refs[: line + 2], refs[line + 2 :]
    project_in(place_ref, pieces, blocks, total_ref, line)
    width = out_ref.shape[1]
    gate = total_ref[:, :width]
    up = total_ref[:, width:]
    out_ref[...] = (gate / (1.0 + jnp.exp(-gate)) * up).astype(out_ref.dtype)


def project_out_kernel(line, place_ref, acts_ref, *refs):
    blocks, outs = refs[: line + 2], refs[line + 2 :]
    rows = outs[0].shape[0]
    depth = blocks[0].shape[0]
    acts = acts_ref[...]
    for k, block in enumerate(block_values(place_ref, blocks, line)):
        start = pl.multiple_of((place_ref[0] ^ k) * depth, depth)
        product = lax.dot_general(
            acts, block, (((1,), (1,)), ((), ())), preferred_element_type=jnp.float32
        ).astype(jnp.bfloat16)
        for n, out_ref in enumerate(outs):
            out_ref[:, pl.ds(start, depth)] = product[n * rows : (n + 1) * rows]


def level_spans(length, core):
    position = lax.iota(jnp.int32, length) ^ (core * (length // 2))
    i, s = position[:, None], position[None, :]
    levels = []
    block = length // 2
    while block >= 1:
        middle = i - i % (2 * block) + block
        after = i >= middle
        query_span = jnp.where(after, (s >= middle) & (s <= i), (s >= i) & (s < middle))
        key_span = jnp.where(after, (s >= middle) & (s < i), (s > i) & (s < middle))
        levels.append(jnp.concatenate([query_span, key_span], axis=0))
        block //= 2
    spans = jnp.stack(levels).astype(jnp.bfloat16)
    return jnp.concatenate([spans, spans], axis=2)


def shards_plane(
    sizes,
    tokens,
    attention_norm_gain,
    query_weight,
    key_weight,
    value_weight,
    decay_weight,
    decay_gate_bias,
    decay_spike_extra,
    head_output_gain,
    output_weight,
    channel_norm_gain,
    gate_weight,
    up_weight,
    down_weight,
):
    n_rep, n_fs, n_tp = sizes
    rep, fs, core = lax.axis_index("rep"), lax.axis_index("fs"), lax.axis_index("tp")
    y, z = fs % 2, fs // 2
    n_seq = 2 * n_rep
    length, width = tokens.shape
    half = length // 2
    depth = query_weight.shape[0]
    slot = rep * 2 + y
    y_slot = rep * 2 + (1 - y)
    middle = jnp.where((z == 0) | (z == LINE - 1), 0, 1)
    place = jnp.stack([fs, middle]).astype(jnp.int32)

    swap_fs = [[(a, a ^ m) for a in range(n_fs)] for m in range(n_fs)]
    mid_pairs = [(a, b) for a, b in swap_fs[6] if a // 2 in (1, 2)]
    end_pairs = [(a, a ^ 2) for a in range(n_fs) if a // 2 in (1, 2)]
    pair_x = [(0, 1), (1, 0)]
    pair_d = [(a * n_fs + b, (1 - a) * n_fs + (b ^ 1)) for a in range(n_rep) for b in range(n_fs)]

    def to_x(v):
        return lax.ppermute(v, "rep", pair_x)

    def to_y(v):
        return lax.ppermute(v, "fs", swap_fs[1])

    def to_d(v):
        return lax.ppermute(v, ("rep", "fs"), pair_d)

    def to_core(v):
        return lax.ppermute(v, "tp", pair_x)

    def columns(weight, index):
        part = weight.shape[1] // n_seq
        return lax.dynamic_slice_in_dim(weight, index * part, part, axis=1)

    def travel(weights):
        own = jnp.concatenate([columns(w, slot) for w in weights], axis=1)
        other = to_y(jnp.concatenate([columns(w, y_slot) for w in weights], axis=1))
        far = [lax.ppermute(v, "fs", swap_fs[4]) for v in (own, other)]
        near = [lax.ppermute(v, "fs", swap_fs[2]) for v in (own, other)]
        by_mid = [lax.ppermute(v, "fs", mid_pairs) for v in (own, other)]
        by_end = [lax.ppermute(v, "fs", end_pairs) for v in far]
        return [own, other, *near, *far, *by_mid, *by_end]

    line = n_fs

    def half_of(v, index):
        return lax.dynamic_slice_in_dim(v, index * half, half, axis=0)

    def gather_rows(mine):
        near = [mine, to_x(mine), to_y(mine), to_d(mine)]
        return near

    in_blocks = travel((query_weight, key_weight, value_weight, decay_weight))
    out_blocks = travel((output_weight,))
    gate_up_blocks = travel((gate_weight, up_weight))
    down_blocks = travel((down_weight,))

    normed = rms_scale(tokens, attention_norm_gain).astype(jnp.bfloat16)
    near = gather_rows(half_of(normed, core))
    far = [half_of(normed, 1 - core)] + [to_core(v) for v in near[1:]]

    n_heads = decay_spike_extra.shape[1]
    heads = n_heads // n_seq
    key_width = query_weight.shape[1] // n_heads
    value_width = value_weight.shape[1] // n_heads
    spike = jnp.concatenate(
        [half_of(decay_spike_extra, core), half_of(decay_spike_extra, 1 - core)], axis=0
    )

    def spike_for(index):
        picked = lax.dynamic_slice_in_dim(spike, index * heads, heads, axis=1)
        return jnp.repeat(picked, key_width, axis=1)

    spikes = [
        spike_for(slot),
        to_x(spike_for((1 - rep) * 2 + y)),
        to_y(spike_for(rep * 2 + 1 - y)),
        to_d(spike_for((1 - rep) * 2 + 1 - y)),
    ]
    wide_k, wide_v = heads * key_width, heads * value_width
    bias = lax.dynamic_slice_in_dim(decay_gate_bias, slot * wide_k, wide_k)[None, :]
    head_gain = jnp.tile(head_output_gain, heads)[None, :]
    n_rows = n_seq * length
    in_width = in_blocks[0].shape[1]
    smem = pl.BlockSpec(memory_space=pltpu.SMEM)
    vmem = pl.BlockSpec(memory_space=pltpu.VMEM)

    def run(body, outs, scratch, operands, flops, name):
        return pl.pallas_call(
            body,
            out_shape=outs,
            in_specs=[smem] + [vmem] * (len(operands) - 1),
            out_specs=jax.tree.map(lambda _: vmem, outs),
            scratch_shapes=scratch,
            compiler_params=pltpu.CompilerParams(vmem_limit_bytes=VMEM_LIMIT),
            cost_estimate=pl.CostEstimate(
                flops=flops,
                bytes_accessed=sum(v.size * v.dtype.itemsize for v in operands),
                transcendentals=0,
            ),
            name=name,
        )(*operands)

    attended = run(
        functools.partial(attention_kernel, line, n_seq, heads, key_width, value_width),
        jax.ShapeDtypeStruct((n_rows, wide_v), jnp.bfloat16),
        [pltpu.VMEM((n_rows, in_width), jnp.float32)],
        [place, *near, *far, *in_blocks, *spikes, level_spans(length, core), bias, head_gain],
        4 * n_rows * width * in_width,
        "attention",
    )

    def project_out(acts, blocks, name):
        shape = jax.ShapeDtypeStruct((half, width), jnp.bfloat16)
        parts = run(
            functools.partial(project_out_kernel, line),
            [shape] * (2 * n_seq),
            [],
            [place, acts, *blocks],
            2 * n_rows * width * acts.shape[1],
            name,
        )
        mine, theirs = parts[:n_seq], parts[n_seq:]
        sums = [
            a.astype(jnp.float32) + to_core(b).astype(jnp.float32) for a, b in zip(mine, theirs)
        ]
        total = sums[0]
        for send, part in zip((to_x, to_y, to_d), sums[1:]):
            total = total + send(part.astype(jnp.bfloat16)).astype(jnp.float32)
        return total

    mixer = project_out(attended, out_blocks, "attention_out")
    residual = (half_of(tokens, core).astype(jnp.float32) + mixer).astype(jnp.bfloat16)
    normed_two = rms_scale(residual, channel_norm_gain).astype(jnp.bfloat16)
    near = gather_rows(normed_two)
    far = [to_core(v) for v in near]
    hidden_width = gate_up_blocks[0].shape[1] // 2
    hidden = run(
        functools.partial(hidden_kernel, line, 2 * n_seq),
        jax.ShapeDtypeStruct((n_rows, hidden_width), jnp.bfloat16),
        [pltpu.VMEM((n_rows, 2 * hidden_width), jnp.float32)],
        [place, *near, *far, *gate_up_blocks],
        4 * n_rows * width * hidden_width,
        "hidden",
    )
    channel = project_out(hidden, down_blocks, "channel_out")
    mine = (residual.astype(jnp.float32) + channel).astype(jnp.bfloat16)
    theirs = to_core(mine)
    first = jnp.where(core == 0, mine, theirs)
    second = jnp.where(core == 0, theirs, mine)
    return jnp.concatenate([first, second], axis=0)


def solution(mesh):
    in_specs = (
        P(("rep", "fs"), None),
        P(),
        P("fs", "tp"),
        P("fs", "tp"),
        P("fs", "tp"),
        P("fs", "tp"),
        P("tp"),
        P(("rep", "fs"), "tp"),
        P(),
        P("fs", "tp"),
        P(),
        P("fs", "tp"),
        P("fs", "tp"),
        P("fs", "tp"),
    )
    out_specs = P(("rep", "fs"), None)
    sizes = tuple(mesh.shape[axis] for axis in ("rep", "fs", "tp"))
    if sizes == (2, 2 * LINE, 2):
        body = functools.partial(shards_plane, sizes)
    else:
        body = shards_general
    return jax.shard_map(body, mesh=mesh, in_specs=in_specs, out_specs=out_specs, check_vma=False)
```
